32 devices in a mesh: fs: 16 (over z, y, core), tp: 2 (over x).
Axes of the slice: x: 2, y: 2, z: 4, core: 2. Of those that a mesh axis runs over, the one named last changes fastest.
Arguments:
- tokens: bfloat16 [16384, 2048], P(('fs', 'tp')), may hold values from -8 to 8
- pre_mix_gain: float32 [2048], replicated, may hold values from 0.1 to 1.9
- post_mix_gain: float32 [2048], replicated, may hold values from 0.1 to 1.9
- pre_ffn_gain: float32 [2048], replicated, may hold values from 0.1 to 1.9
- post_ffn_gain: float32 [2048], replicated, may hold values from 0.1 to 1.9
- w_branch: bfloat16 [2048, 1024], P('fs', 'tp'), may hold values from -0.125 to 0.125
- w_gelu: bfloat16 [2048, 1024], P('fs', 'tp'), may hold values from -0.125 to 0.125
- conv_weight: bfloat16 [4, 1024], P(None, 'tp'), may hold values from -3 to 3
- w_rec: bfloat16 [2, 8, 128, 128], P(None, 'tp'), may hold values from -0.5 to 0.5
- w_inp: bfloat16 [2, 8, 128, 128], P(None, 'tp'), may hold values from -0.5 to 0.5
- decay: float32 [2, 1024], P(None, 'tp'), may hold values from 3 to 10
- out_weight_t: bfloat16 [2048, 1024], P('fs', 'tp'), may hold values from -0.1875 to 0.1875
- w_gate: bfloat16 [2048, 3072], P('fs', 'tp'), may hold values from -0.125 to 0.125
- w_up: bfloat16 [2048, 3072], P('fs', 'tp'), may hold values from -0.125 to 0.125
- down_weight_t: bfloat16 [2048, 3072], P('fs', 'tp'), may hold values from -0.109375 to 0.109375
Outputs:
- layer_out: bfloat16 [16384, 2048], P(('fs', 'tp'))
The draws below stay inside these ranges and needn't reach their ends.
All inputs are finite; a program needn't handle non-finite values.
Results may differ from the reference program's by a relative error of at most 0.014.
Values may be sent and summed in bfloat16 or wider, within the bound.
No kernel may reach another device: no remote copies, remote signals or barrier semaphores. Data moves between devices by JAX's collectives and lax.ppermute only.
A program may use at most 128 MiB of HBM per device.

```python
import math
import jax
import jax.numpy as jnp
from jax import lax

D = 2048
BLOCKS = 8
BW = 128
FF = 3072
SEQ_LEN = 1024
D_LRU = 1024
TOKENS = 16384
N_FS = 16
N_TP = 2


def draw_tokens(key, part):
    noise_key = jax.random.fold_in(key, 11)
    common_key = jax.random.fold_in(key, 12)
    block_count = (TOKENS + 15) // 16
    block_index = jnp.arange(TOKENS) // 16
    common = jax.random.normal(common_key, (block_count, D), jnp.float32)
    noise = jax.random.normal(noise_key, (TOKENS, D), jnp.float32)
    values = noise + 1.2 * common[block_index]
    return jnp.clip(values, -8.0, 8.0).astype(jnp.bfloat16)


def draw_decay(key, part):
    choose_key = jax.random.fold_in(key, 21)
    slow_key = jax.random.fold_in(key, 22)
    fast_key = jax.random.fold_in(key, 23)
    fast_share = 0.5
    fast = jax.random.uniform(choose_key, (2, D_LRU), jnp.float32) < fast_share
    slow_rate = jnp.exp(jax.random.uniform(slow_key, (2, D_LRU), jnp.float32, math.log(0.3), math.log(1.5))) / SEQ_LEN
    fast_rate = 1.0 / jnp.exp(jax.random.uniform(fast_key, (2, D_LRU), jnp.float32, math.log(15.0), math.log(50.0)))
    per_step = jnp.where(fast, fast_rate, slow_rate)
    return (-jnp.log(jnp.expm1(per_step / 4.0))).astype(jnp.float32)


def steps_of(rng, shape, cuts, smallest, high):
    level, own = 1.0, jax.random.fold_in(rng, 6)
    for dim, blocks in cuts:
        steps = jnp.exp(jax.random.uniform(jax.random.fold_in(own, dim), (blocks,), jnp.float32, smallest / len(cuts), high / len(cuts)))
        level = level * jnp.repeat(steps, shape[dim] // blocks).reshape([-1 if axis == dim else 1 for axis in range(len(shape))])
    return level


def gaussian(own_key, dims, deviation, reach, split=(), held_as=jnp.bfloat16):
    values = deviation * jax.random.normal(own_key, dims, jnp.float32)
    if split:
        values = values * steps_of(own_key, dims, split, -0.22, 0.18)
    return jnp.clip(values, -reach, reach).astype(held_as)


def setup_inputs(seed: int = 0) -> dict:
    key_list = jax.random.split(jax.random.key(seed), 16)
    return {
        "tokens": draw_tokens(jax.random.fold_in(key_list[15], 71), 0),
        "pre_mix_gain": jnp.clip(1.0 + 0.18 * jax.random.normal(key_list[1], (D,), jnp.float32), 0.1, 1.9),
        "post_mix_gain": jnp.clip(1.0 + 0.18 * jax.random.normal(key_list[2], (D,), jnp.float32), 0.1, 1.9),
        "pre_ffn_gain": jnp.clip(1.0 + 0.18 * jax.random.normal(key_list[3], (D,), jnp.float32), 0.1, 1.9),
        "post_ffn_gain": jnp.clip(1.0 + 0.18 * jax.random.normal(key_list[4], (D,), jnp.float32), 0.1, 1.9),
        "w_branch": gaussian(key_list[5], (D, D_LRU), D ** -0.5, 0.125, ((0, 16), (1, 2))),
        "w_gelu": gaussian(key_list[6], (D, D_LRU), D ** -0.5, 0.125, ((0, 16), (1, 2))),
        "conv_weight": gaussian(key_list[7], (4, D_LRU), 0.5, 3.0, ((1, 2),)),
        "w_rec": gaussian(key_list[8], (2, BLOCKS, BW, BW), BW ** -0.5, 0.5, ((1, 2),)),
        "w_inp": gaussian(key_list[9], (2, BLOCKS, BW, BW), BW ** -0.5, 0.5, ((1, 2),)),
        "decay": draw_decay(jax.random.fold_in(key_list[15], 71), 0),
        "out_weight_t": gaussian(key_list[11], (D, D_LRU), D_LRU ** -0.5, 0.1875, ((0, 16), (1, 2))),
        "w_gate": gaussian(key_list[12], (D, FF), D ** -0.5, 0.125, ((0, 16), (1, 2))),
        "w_up": gaussian(key_list[13], (D, FF), D ** -0.5, 0.125, ((0, 16), (1, 2))),
        "down_weight_t": gaussian(key_list[14], (D, FF), FF ** -0.5, 0.109375, ((0, 16), (1, 2))),
    }


EPS = 1e-06

def normed(values, gain):
    factor = lax.rsqrt(lax.optimization_barrier(jnp.mean(values * values, axis=-1, keepdims=True)) + EPS)
    return values * factor * gain

def conv_short(branch, conv_weight):
    length = branch.shape[0]
    padded = jnp.pad(branch.astype(jnp.float32), ((2, 1), (0, 0)))
    weights = conv_weight.astype(jnp.float32)
    summed = weights[0] * padded[0:length]
    for offset in range(1, 4):
        summed = summed + weights[offset] * padded[offset:offset + length]
    return summed.astype(jnp.bfloat16)

def combine(earlier, later):
    return (earlier[0] * later[0], later[0] * earlier[1] + later[1])

def recurrence(conv_out, w_rec, w_inp, decay):
    length, channels = conv_out.shape
    blocks = w_rec.shape[0]
    grouped = conv_out.astype(jnp.float32).reshape(length, blocks, channels // blocks)
    rate_gate = jax.nn.sigmoid(jnp.einsum('lnc,ncd->lnd', grouped, w_rec.astype(jnp.float32)).reshape(length, channels))
    inflow = jax.nn.sigmoid(jnp.einsum('lnc,ncd->lnd', grouped, w_inp.astype(jnp.float32)).reshape(length, channels))
    log_retain = -8.0 * rate_gate * jax.nn.softplus(-decay)
    retain = jnp.exp(log_retain)
    feed = jnp.sqrt(-jnp.expm1(2.0 * log_retain)) * inflow * conv_out.astype(jnp.float32)
    unused_decay, states = lax.associative_scan(combine, (retain, feed), axis=0)
    return states

def grouped_sum(hidden, weight_t):
    group_cols = hidden.shape[1] // N_TP

    def add_group(index, summed):
        first_col = (index * group_cols).astype(jnp.int32)
        part_rows = lax.dynamic_slice_in_dim(hidden, first_col, group_cols, 1)
        part_cols = lax.dynamic_slice_in_dim(weight_t, first_col, group_cols, 1)
        partial_value = lax.dot_general(part_rows, part_cols, (((1,), (1,)), ((), ())), preferred_element_type=jnp.float32)
        rounded = lax.optimization_barrier(partial_value.astype(jnp.bfloat16))
        return summed + rounded.astype(jnp.float32)
    zero_block = jnp.zeros((hidden.shape[0], weight_t.shape[0]), jnp.float32)
    return lax.fori_loop(0, N_TP, add_group, zero_block)

def reference(tokens, pre_mix_gain, post_mix_gain, pre_ffn_gain, post_ffn_gain, w_branch, w_gelu, conv_weight, w_rec, w_inp, decay, out_weight_t, w_gate, w_up, down_weight_t):

    def one_sequence(seq_tokens):
        stream = seq_tokens.astype(jnp.float32)
        normed_in = normed(stream, pre_mix_gain).astype(jnp.bfloat16)
        branch_in = jnp.dot(normed_in, w_branch, preferred_element_type=jnp.float32).astype(jnp.bfloat16)
        gelu_in = jnp.dot(normed_in, w_gelu, preferred_element_type=jnp.float32).astype(jnp.bfloat16)
        conv_out = conv_short(branch_in, conv_weight)
        forward = recurrence(conv_out, w_rec[0], w_inp[0], decay[0])
        backward = jnp.flip(recurrence(jnp.flip(conv_out, 0), w_rec[1], w_inp[1], decay[1]), 0)
        mixer_hidden = (jax.nn.gelu(gelu_in.astype(jnp.float32)) * (forward + backward)).astype(jnp.bfloat16)
        mixer_sum = lax.dot_general(mixer_hidden, out_weight_t, (((1,), (1,)), ((), ())), preferred_element_type=jnp.float32)
        residual = (stream + normed(mixer_sum, post_mix_gain)).astype(jnp.bfloat16)
        middle = residual.astype(jnp.float32)
        normed_mid = normed(middle, pre_ffn_gain).astype(jnp.bfloat16)
        gate_proj = jnp.dot(normed_mid, w_gate, preferred_element_type=jnp.float32)
        up_proj = jnp.dot(normed_mid, w_up, preferred_element_type=jnp.float32)
        ffn_hidden = (jax.nn.silu(gate_proj) * up_proj).astype(jnp.bfloat16)
        ffn_sum = grouped_sum(ffn_hidden, down_weight_t)
        return (middle + normed(ffn_sum, post_ffn_gain)).astype(jnp.bfloat16)
    sequences = tokens.reshape(N_FS, SEQ_LEN, D)
    outputs = lax.map(one_sequence, sequences)
    return outputs.reshape(N_FS * SEQ_LEN, D)
```

```python
import functools

import jax
import jax.numpy as jnp
from jax import lax
from jax.experimental import pallas as pl
from jax.experimental.pallas import tpu as pltpu
from jax.sharding import PartitionSpec as P

EPS = 1e-06
SEGMENTS = 8
LANES = 128
F32 = jnp.float32
BF16 = jnp.bfloat16


def normed(values, gain):
    factor = lax.rsqrt(jnp.mean(values * values, axis=-1, keepdims=True) + EPS)
    return values * factor * gain


def tile_of(size, limit):
    tile = min(size, limit)
    while size % tile:
        tile -= LANES
    return tile


def one_minus_exp(y):
    series = 1.0 + y * (1.0 / 6.0)
    for term in (5.0, 4.0, 3.0, 2.0):
        series = 1.0 + y * (1.0 / term) * series
    return jnp.where(y > -0.25, -y * series, 1.0 - jnp.exp(y))


def dot_nn(left, right):
    return jnp.dot(left, right, preferred_element_type=F32)


def dot_nt(left, right):
    return lax.dot_general(left, right, (((1,), (1,)), ((), ())), preferred_element_type=F32)


def mixer_kernel(
    place_ref, own_ref, other_ref, wb_ref, wg_ref, cw_ref, rec_ref, inp_ref, slope_ref,
    mine_ref, theirs_ref, branch_ref, gelu_ref, a0, b0, a1, b1, hf, hb,
):
    half = own_ref.shape[0]
    length = 2 * half
    steps = length // SEGMENTS
    blocks = rec_ref.shape[1]
    own_at = pl.multiple_of(place_ref[0] * half, half)
    other_at = pl.multiple_of((1 - place_ref[0]) * half, half)
    for source, start in ((own_ref, own_at), (other_ref, other_at)):
        rows = source[...]
        branch_ref[pl.ds(start, half), :] = dot_nn(rows, wb_ref[...]).astype(BF16).astype(F32)
        gelu_ref[pl.ds(start, half), :] = dot_nn(rows, wg_ref[...]).astype(BF16)
    row = lax.broadcasted_iota(jnp.int32, (length, LANES), 0)
    for block in range(blocks):
        cols = slice(block * LANES, (block + 1) * LANES)
        branch = branch_ref[:, cols]
        taps = cw_ref[:, cols].astype(F32)
        summed = taps[0:1] * jnp.where(row >= 2, pltpu.roll(branch, 2, 0), 0.0)
        summed = summed + taps[1:2] * jnp.where(row >= 1, pltpu.roll(branch, 1, 0), 0.0)
        summed = summed + taps[2:3] * branch
        summed = summed + taps[3:4] * jnp.where(
            row < length - 1, pltpu.roll(branch, length - 1, 0), 0.0
        )
        conv = summed.astype(BF16)
        conv_wide = conv.astype(F32)
        for direction, (a_ref, b_ref) in enumerate(((a0, b0), (a1, b1))):
            rate = jax.nn.sigmoid(dot_nn(conv, rec_ref[direction, block]))
            inflow = jax.nn.sigmoid(dot_nn(conv, inp_ref[direction, block]))
            log_a = rate * slope_ref[direction : direction + 1, cols]
            a_ref[block] = jnp.exp(log_a)
            b_ref[block] = jnp.sqrt(one_minus_exp(2.0 * log_a)) * inflow * conv_wide

    def at(step):
        return pl.ds(step, SEGMENTS, stride=steps)

    def advance(step, states, store):
        new = []
        back = steps - 1 - step
        for block in range(blocks):
            for ar, br, hr, where in ((a0, b0, hf, step), (a1, b1, hb, back)):
                state, product = states[len(new)]
                keep = ar[block, at(where), :]
                state = keep * state + br[block, at(where), :]
                if store:
                    hr[block, at(where), :] = state
                else:
                    product = product * keep
                new.append((state, product))
        return tuple(new)

    zero = jnp.zeros((SEGMENTS, LANES), F32)
    one = jnp.ones((SEGMENTS, LANES), F32)
    ends = lax.fori_loop(
        0, steps, lambda i, s: advance(i, s, False), ((zero, one),) * (2 * blocks), unroll=8
    )
    starts = []
    for index, (state, product) in enumerate(ends):
        order = list(range(SEGMENTS))
        if index % 2:
            order = order[::-1]
        rows = [None] * SEGMENTS
        carry = zero[0:1]
        for segment in order:
            rows[segment] = carry
            carry = state[segment : segment + 1] + product[segment : segment + 1] * carry
        starts.append((jnp.concatenate(rows, axis=0), zero))
    lax.fori_loop(0, steps, lambda i, s: advance(i, s, True), tuple(starts), unroll=8)
    for target, start in ((mine_ref, own_at), (theirs_ref, other_at)):
        for block in range(blocks):
            cols = slice(block * LANES, (block + 1) * LANES)
            states = hf[block, pl.ds(start, half), :] + hb[block, pl.ds(start, half), :]
            factor = jax.nn.gelu(gelu_ref[pl.ds(start, half), cols].astype(F32))
            target[:, cols] = (factor * states).astype(BF16)


def mixer(place, own, other, gathered, conv_weight, w_rec, w_inp, slope):
    half, width = own.shape
    channels = conv_weight.shape[1]
    group = tile_of(channels, 2 * LANES)
    blocks = group // LANES
    count = channels // group
    length = 2 * half
    wide = pltpu.VMEM((blocks, length, LANES), F32)
    whole = pl.BlockSpec((half, width), lambda j: (0, 0))
    maps = pl.BlockSpec((2, blocks, LANES, LANES), lambda j: (0, j, 0, 0))
    piece = pl.BlockSpec((half, group), lambda j: (0, j))
    return pl.pallas_call(
        mixer_kernel,
        grid=(count,),
        in_specs=[
            pl.BlockSpec(memory_space=pltpu.SMEM),
            whole,
            whole,
            pl.BlockSpec((width, group), lambda j: (0, j)),
            pl.BlockSpec((width, group), lambda j: (0, count + j)),
            pl.BlockSpec((conv_weight.shape[0], group), lambda j: (0, j)),
            maps,
            maps,
            pl.BlockSpec((2, group), lambda j: (0, j)),
        ],
        out_specs=[piece, piece],
        out_shape=[jax.ShapeDtypeStruct((half, channels), BF16)] * 2,
        scratch_shapes=[
            pltpu.VMEM((length, group), F32),
            pltpu.VMEM((length, group), BF16),
            wide, wide, wide, wide, wide, wide,
        ],
        compiler_params=pltpu.CompilerParams(vmem_limit_bytes=56 * 2**20),
        name="mixer",
    )(place, own, other, gathered, gathered, conv_weight, w_rec, w_inp, slope)


def out_kernel(ha_ref, hb_ref, wa_ref, wb_ref, tok_ref, gain_ref, mid_gain_ref, res_ref, mid_ref):
    summed = dot_nt(ha_ref[...], wa_ref[...]) + dot_nt(hb_ref[...], wb_ref[...])
    residual = (tok_ref[...].astype(F32) + normed(summed, gain_ref[...])).astype(BF16)
    res_ref[...] = residual
    mid_ref[...] = normed(residual.astype(F32), mid_gain_ref[...]).astype(BF16)


def out_projection(ha, hb, wa, wa_block, wb, wb_block, tokens, gain, mid_gain):
    rows, width = tokens.shape
    tile = min(rows, 256)
    channels = ha.shape[1]
    hidden = pl.BlockSpec((tile, channels), lambda i: (i, 0))
    wide = pl.BlockSpec((tile, width), lambda i: (i, 0))
    gains = pl.BlockSpec((1, width), lambda i: (0, 0))
    return pl.pallas_call(
        out_kernel,
        grid=(rows // tile,),
        in_specs=[
            hidden,
            hidden,
            pl.BlockSpec((width, channels), lambda i: (0, wa_block)),
            pl.BlockSpec((width, channels), lambda i: (0, wb_block)),
            wide,
            gains,
            gains,
        ],
        out_specs=[wide, wide],
        out_shape=[jax.ShapeDtypeStruct((rows, width), BF16)] * 2,
        compiler_params=pltpu.CompilerParams(vmem_limit_bytes=56 * 2**20),
        name="out_projection",
    )(ha, hb, wa, wb, tokens, gain[None], mid_gain[None])


def ffn_kernel(x_ref, gate_ref, up_ref, down_ref, out_ref, acc_ref):
    rows = x_ref[...]
    gate = dot_nn(rows, gate_ref[...])
    hidden = (gate * jax.nn.sigmoid(gate) * dot_nn(rows, up_ref[...])).astype(BF16)
    partial = dot_nt(hidden, down_ref[...])
    step = pl.program_id(0)
    last = pl.num_programs(0) - 1

    @pl.when(step == 0)
    def _():
        acc_ref[...] = partial

    @pl.when(step > 0)
    def _():
        acc_ref[...] += partial

    @pl.when(step == last)
    def _():
        out_ref[...] = acc_ref[...].astype(BF16)


def ffn(rows, gathered):
    count, width = rows.shape
    hidden_units = gathered.shape[1] // 3
    tile = tile_of(hidden_units, 512)
    tiles = hidden_units // tile
    whole = pl.BlockSpec((count, width), lambda j: (0, 0))
    return pl.pallas_call(
        ffn_kernel,
        grid=(tiles,),
        in_specs=[
            whole,
            pl.BlockSpec((width, tile), lambda j: (0, j)),
            pl.BlockSpec((width, tile), lambda j: (0, tiles + j)),
            pl.BlockSpec((width, tile), lambda j: (0, 2 * tiles + j)),
        ],
        out_specs=whole,
        out_shape=jax.ShapeDtypeStruct((count, width), BF16),
        scratch_shapes=[pltpu.VMEM((count, width), F32)],
        compiler_params=pltpu.CompilerParams(vmem_limit_bytes=56 * 2**20),
        name="ffn",
    )(rows, gathered, gathered, gathered)


def per_device(
    ranks,
    tokens,
    pre_mix_gain,
    post_mix_gain,
    pre_ffn_gain,
    post_ffn_gain,
    w_branch,
    w_gelu,
    conv_weight,
    w_rec,
    w_inp,
    decay,
    out_weight_t,
    w_gate,
    w_up,
    down_weight_t,
):
    swap = [(0, 1), (1, 0)]
    rows = tokens.shape[0]
    mix_shard = jnp.concatenate([w_branch, w_gelu, out_weight_t], axis=1)
    ffn_shard = jnp.concatenate([w_gate, w_up, down_weight_t], axis=1)
    mix_all = lax.all_gather(mix_shard, "fs", axis=0, tiled=True)
    mix_all, ffn_shard = lax.optimization_barrier((mix_all, ffn_shard))
    ffn_all = lax.all_gather(ffn_shard, "fs", axis=0, tiled=True)
    channels = w_branch.shape[1]
    stream = tokens.astype(F32)
    normed_in = normed(stream, pre_mix_gain).astype(BF16)
    slope = -8.0 * jax.nn.softplus(-decay)
    place = lax.axis_index("tp").astype(jnp.int32).reshape(1)
    if ranks == 2:
        other_in = lax.ppermute(normed_in, "tp", swap)
        out_other = lax.ppermute(mix_all[:, 2 * channels :], "tp", swap)
        mine, theirs = mixer(
            place, normed_in, other_in, mix_all, conv_weight, w_rec, w_inp, slope
        )
        received = lax.ppermute(theirs, "tp", swap)
        residual, normed_mid = out_projection(
            mine, received, mix_all, 2, out_other, 0, tokens, post_mix_gain, pre_ffn_gain
        )
        other_mid = lax.ppermute(normed_mid, "tp", swap)
        pieces = 2 if rows % 512 == 0 else 1
        size = rows // pieces
        returned = []
        for piece in range(pieces):
            part = ffn(lax.slice_in_dim(other_mid, piece * size, (piece + 1) * size), ffn_all)
            returned.append(lax.ppermute(part, "tp", swap))
        own_part = ffn(normed_mid, ffn_all)
        ffn_sum = own_part.astype(F32) + jnp.concatenate(returned, axis=0).astype(F32)
    else:
        everything = lax.all_gather(normed_in, "tp", axis=0, tiled=True)
        half = everything.shape[0] // 2
        first, second = mixer(
            place * 0, everything[:half], everything[half:], mix_all, conv_weight, w_rec, w_inp, slope
        )
        hidden = lax.all_to_all(
            jnp.concatenate([first, second], axis=0), "tp", split_axis=0, concat_axis=1, tiled=True
        )
        out_whole = lax.all_gather(mix_all[:, 2 * channels :], "tp", axis=1, tiled=True)
        mid_cols = hidden.shape[1] // 2
        residual, normed_mid = out_projection(
            hidden[:, :mid_cols], hidden[:, mid_cols:], out_whole, 0, out_whole, 1,
            tokens, post_mix_gain, pre_ffn_gain,
        )
        every_mid = lax.all_gather(normed_mid, "tp", axis=0, tiled=True)
        ffn_sum = lax.psum_scatter(
            ffn(every_mid, ffn_all), "tp", scatter_dimension=0, tiled=True
        ).astype(F32)
    return (residual.astype(F32) + normed(ffn_sum, post_ffn_gain)).astype(BF16)


def solution(mesh):
    return jax.shard_map(
        functools.partial(per_device, mesh.shape["tp"]),
        mesh=mesh,
        in_specs=(
            P(("fs", "tp"), None),
            P(),
            P(),
            P(),
            P(),
            P("fs", "tp"),
            P("fs", "tp"),
            P(None, "tp"),
            P(None, "tp", None, None),
            P(None, "tp", None, None),
            P(None, "tp"),
            P("fs", "tp"),
            P("fs", "tp"),
            P("fs", "tp"),
            P("fs", "tp"),
        ),
        out_specs=P(("fs", "tp"), None),
        check_vma=False,
    )
```

```python
import functools

import jax
import jax.numpy as jnp
from jax import lax
from jax.experimental import pallas as pl
from jax.experimental.pallas import tpu as pltpu
from jax.sharding import PartitionSpec as P

EPS = 1e-06
SEGMENTS = 8
LANES = 128
F32 = jnp.float32
BF16 = jnp.bfloat16


def normed(values, gain):
    factor = lax.rsqrt(jnp.mean(values * values, axis=-1, keepdims=True) + EPS)
    return values * factor * gain


def tile_of(size, limit):
    tile = min(size, limit)
    while size % tile:
        tile -= LANES
    return tile


def cost(flops):
    return pl.CostEstimate(flops=flops, bytes_accessed=flops // 256, transcendentals=0)


def one_minus_exp(y):
    series = 1.0 + y * (1.0 / 6.0)
    for term in (5.0, 4.0, 3.0, 2.0):
        series = 1.0 + y * (1.0 / term) * series
    return jnp.where(y > -0.25, -y * series, 1.0 - jnp.exp(y))


def dot_nn(left, right):
    return jnp.dot(left, right, preferred_element_type=F32)


def dot_nt(left, right):
    return lax.dot_general(left, right, (((1,), (1,)), ((), ())), preferred_element_type=F32)


def mixer_kernel(
    place_ref, own_ref, other_ref, wb_ref, wg_ref, cw_ref, rec_ref, inp_ref, slope_ref,
    mine_ref, theirs_ref, branch_ref, gelu_ref, a0, b0, a1, b1, hf, hb,
):
    half = own_ref.shape[0]
    length = 2 * half
    steps = length // SEGMENTS
    blocks = rec_ref.shape[1]
    own_at = pl.multiple_of(place_ref[0] * half, half)
    other_at = pl.multiple_of((1 - place_ref[0]) * half, half)
    for source, start in ((own_ref, own_at), (other_ref, other_at)):
        rows = source[...]
        branch_ref[pl.ds(start, half), :] = dot_nn(rows, wb_ref[...]).astype(BF16).astype(F32)
        gelu_ref[pl.ds(start, half), :] = dot_nn(rows, wg_ref[...]).astype(BF16)
    row = lax.broadcasted_iota(jnp.int32, (length, LANES), 0)
    for block in range(blocks):
        cols = slice(block * LANES, (block + 1) * LANES)
        branch = branch_ref[:, cols]
        taps = cw_ref[:, cols].astype(F32)
        summed = taps[0:1] * jnp.where(row >= 2, pltpu.roll(branch, 2, 0), 0.0)
        summed = summed + taps[1:2] * jnp.where(row >= 1, pltpu.roll(branch, 1, 0), 0.0)
        summed = summed + taps[2:3] * branch
        summed = summed + taps[3:4] * jnp.where(
            row < length - 1, pltpu.roll(branch, length - 1, 0), 0.0
        )
        conv = summed.astype(BF16)
        conv_wide = conv.astype(F32)
        for direction, (a_ref, b_ref) in enumerate(((a0, b0), (a1, b1))):
            rate = jax.nn.sigmoid(dot_nn(conv, rec_ref[direction, block]))
            inflow = jax.nn.sigmoid(dot_nn(conv, inp_ref[direction, block]))
            log_a = rate * slope_ref[direction : direction + 1, cols]
            a_ref[block] = jnp.exp(log_a)
            b_ref[block] = jnp.sqrt(one_minus_exp(2.0 * log_a)) * inflow * conv_wide

    def at(step):
        return pl.ds(step, SEGMENTS, stride=steps)

    def advance(step, states, store):
        new = []
        back = steps - 1 - step
        for block in range(blocks):
            for ar, br, hr, where in ((a0, b0, hf, step), (a1, b1, hb, back)):
                state, product = states[len(new)]
                keep = ar[block, at(where), :]
                state = keep * state + br[block, at(where), :]
                if store:
                    hr[block, at(where), :] = state
                else:
                    product = product * keep
                new.append((state, product))
        return tuple(new)

    zero = jnp.zeros((SEGMENTS, LANES), F32)
    one = jnp.ones((SEGMENTS, LANES), F32)
    ends = lax.fori_loop(
        0, steps, lambda i, s: advance(i, s, False), ((zero, one),) * (2 * blocks), unroll=8
    )
    starts = []
    for index, (state, product) in enumerate(ends):
        order = list(range(SEGMENTS))
        if index % 2:
            order = order[::-1]
        rows = [None] * SEGMENTS
        carry = zero[0:1]
        for segment in order:
            rows[segment] = carry
            carry = state[segment : segment + 1] + product[segment : segment + 1] * carry
        starts.append((jnp.concatenate(rows, axis=0), zero))
    lax.fori_loop(0, steps, lambda i, s: advance(i, s, True), tuple(starts), unroll=8)
    for target, start in ((mine_ref, own_at), (theirs_ref, other_at)):
        for block in range(blocks):
            cols = slice(block * LANES, (block + 1) * LANES)
            states = hf[block, pl.ds(start, half), :] + hb[block, pl.ds(start, half), :]
            factor = jax.nn.gelu(gelu_ref[pl.ds(start, half), cols].astype(F32))
            target[:, cols] = (factor * states).astype(BF16)


def mixer(place, own, other, gathered, conv_weight, w_rec, w_inp, slope):
    half, width = own.shape
    channels = conv_weight.shape[1]
    group = tile_of(channels, 2 * LANES)
    blocks = group // LANES
    count = channels // group
    length = 2 * half
    wide = pltpu.VMEM((blocks, length, LANES), F32)
    whole = pl.BlockSpec((half, width), lambda j: (0, 0))
    maps = pl.BlockSpec((2, blocks, LANES, LANES), lambda j: (0, j, 0, 0))
    piece = pl.BlockSpec((half, group), lambda j: (0, j))
    return pl.pallas_call(
        mixer_kernel,
        grid=(count,),
        in_specs=[
            pl.BlockSpec(memory_space=pltpu.SMEM),
            whole,
            whole,
            pl.BlockSpec((width, group), lambda j: (0, j)),
            pl.BlockSpec((width, group), lambda j: (0, count + j)),
            pl.BlockSpec((conv_weight.shape[0], group), lambda j: (0, j)),
            maps,
            maps,
            pl.BlockSpec((2, group), lambda j: (0, j)),
        ],
        out_specs=[piece, piece],
        out_shape=[jax.ShapeDtypeStruct((half, channels), BF16)] * 2,
        scratch_shapes=[
            pltpu.VMEM((length, group), F32),
            pltpu.VMEM((length, group), BF16),
            wide, wide, wide, wide, wide, wide,
        ],
        compiler_params=pltpu.CompilerParams(vmem_limit_bytes=56 * 2**20),
        cost_estimate=cost(32 * length * width * channels),
        name="mixer",
    )(place, own, other, gathered, gathered, conv_weight, w_rec, w_inp, slope)


def out_kernel(
    ha_ref, hb_ref, wa_ref, wlow_ref, whigh_ref, tok_ref, gain_ref, mid_gain_ref, res_ref, mid_ref
):
    second = hb_ref[...]
    summed = dot_nt(ha_ref[...], wa_ref[...]) + jnp.concatenate(
        [dot_nt(second, wlow_ref[...]), dot_nt(second, whigh_ref[...])], axis=1
    )
    residual = (tok_ref[...].astype(F32) + normed(summed, gain_ref[...])).astype(BF16)
    res_ref[...] = residual
    mid_ref[...] = normed(residual.astype(F32), mid_gain_ref[...]).astype(BF16)


def out_projection(ha, hb, wa, wa_block, wlow, wb_block, whigh, tokens, gain, mid_gain):
    rows, width = tokens.shape
    tile = min(rows, 256)
    channels = ha.shape[1]
    hidden = pl.BlockSpec((tile, channels), lambda i: (i, 0))
    wide = pl.BlockSpec((tile, width), lambda i: (i, 0))
    gains = pl.BlockSpec((1, width), lambda i: (0, 0))
    return pl.pallas_call(
        out_kernel,
        grid=(rows // tile,),
        in_specs=[
            hidden,
            hidden,
            pl.BlockSpec((width, channels), lambda i: (0, wa_block)),
            pl.BlockSpec((width // 2, channels), lambda i: (0, wb_block)),
            pl.BlockSpec((width // 2, channels), lambda i: (0, wb_block)),
            wide,
            gains,
            gains,
        ],
        out_specs=[wide, wide],
        out_shape=[jax.ShapeDtypeStruct((rows, width), BF16)] * 2,
        compiler_params=pltpu.CompilerParams(vmem_limit_bytes=56 * 2**20),
        cost_estimate=cost(16 * rows * width * channels),
        name="out_projection",
    )(ha, hb, wa, wlow, whigh, tokens, gain[None], mid_gain[None])


def ffn_kernel(x_ref, gate_ref, up_ref, down_ref, out_ref, acc_ref):
    rows = x_ref[...]
    gate = dot_nn(rows, gate_ref[...])
    hidden = (gate * jax.nn.sigmoid(gate) * dot_nn(rows, up_ref[...])).astype(BF16)
    partial = dot_nt(hidden, down_ref[...])
    step = pl.program_id(0)
    last = pl.num_programs(0) - 1

    @pl.when(step == 0)
    def _():
        acc_ref[...] = partial

    @pl.when(step > 0)
    def _():
        acc_ref[...] += partial

    @pl.when(step == last)
    def _():
        out_ref[...] = acc_ref[...].astype(BF16)


def ffn(rows, gathered):
    count, width = rows.shape
    hidden_units = gathered.shape[1] // 3
    tile = tile_of(hidden_units, 512)
    tiles = hidden_units // tile
    whole = pl.BlockSpec((count, width), lambda j: (0, 0))
    return pl.pallas_call(
        ffn_kernel,
        grid=(tiles,),
        in_specs=[
            whole,
            pl.BlockSpec((width, tile), lambda j: (0, j)),
            pl.BlockSpec((width, tile), lambda j: (0, tiles + j)),
            pl.BlockSpec((width, tile), lambda j: (0, 2 * tiles + j)),
        ],
        out_specs=whole,
        out_shape=jax.ShapeDtypeStruct((count, width), BF16),
        scratch_shapes=[pltpu.VMEM((count, width), F32)],
        compiler_params=pltpu.CompilerParams(vmem_limit_bytes=56 * 2**20),
        cost_estimate=cost(6 * count * width * hidden_units),
        name="ffn",
    )(rows, gathered, gathered, gathered)


def finish_kernel(res_ref, own_ref, back_ref, gain_ref, *refs):
    summed = own_ref[...].astype(F32) + back_ref[...].astype(F32)
    layer = res_ref[...].astype(F32) + normed(summed, gain_ref[...])
    refs[-1][...] = layer.astype(BF16)


def finish(residual, own, back, gain, piece, earlier):
    size, width = back.shape
    tile = min(size, LANES)
    tiles = size // tile
    placed = pl.BlockSpec((tile, width), lambda i: (piece * tiles + i, 0))
    operands = [residual, own, back, gain[None]]
    specs = [
        placed,
        placed,
        pl.BlockSpec((tile, width), lambda i: (i, 0)),
        pl.BlockSpec((1, width), lambda i: (0, 0)),
    ]
    aliases = {}
    if earlier is not None:
        aliases = {len(operands): 0}
        operands.append(earlier)
        specs.append(pl.BlockSpec(memory_space=pl.ANY))
    return pl.pallas_call(
        finish_kernel,
        grid=(tiles,),
        in_specs=specs,
        out_specs=placed,
        out_shape=jax.ShapeDtypeStruct(residual.shape, BF16),
        input_output_aliases=aliases,
        name="finish",
    )(*operands)


def per_device(
    ranks,
    fs_size,
    tokens,
    pre_mix_gain,
    post_mix_gain,
    pre_ffn_gain,
    post_ffn_gain,
    w_branch,
    w_gelu,
    conv_weight,
    w_rec,
    w_inp,
    decay,
    out_weight_t,
    w_gate,
    w_up,
    down_weight_t,
):
    swap = [(0, 1), (1, 0)]
    rows = tokens.shape[0]
    mix_shard = jnp.concatenate([w_branch, w_gelu, out_weight_t], axis=1)
    ffn_shard = jnp.concatenate([w_gate, w_up, down_weight_t], axis=1)
    mix_all = lax.all_gather(mix_shard, "fs", axis=0, tiled=True)
    channels = w_branch.shape[1]
    stream = tokens.astype(F32)
    normed_in = normed(stream, pre_mix_gain).astype(BF16)
    if ranks == 2:
        other_in = lax.ppermute(normed_in, "tp", swap)
        mix_all, ffn_shard, other_in = lax.optimization_barrier((mix_all, ffn_shard, other_in))
    else:
        mix_all, ffn_shard = lax.optimization_barrier((mix_all, ffn_shard))
    ffn_all = lax.all_gather(ffn_shard, "fs", axis=0, tiled=True)
    slope = -8.0 * jax.nn.softplus(-decay)
    place = lax.axis_index("tp").astype(jnp.int32).reshape(1)
    if ranks == 2:
        lanes_at = 2 * channels
        width = mix_all.shape[0]
        pairs = fs_size % 2 == 0
        if pairs:
            part = lax.axis_index("fs").astype(jnp.int32) % 2
            out_half = lax.dynamic_slice(
                mix_all, (part * (width // 2), lanes_at), (width // 2, channels)
            )
        else:
            out_half = mix_all[:, lanes_at:]
        out_half = lax.ppermute(out_half, "tp", swap)
        mine, theirs = mixer(
            place, normed_in, other_in, mix_all, conv_weight, w_rec, w_inp, slope
        )
        received = lax.ppermute(theirs, "tp", swap)
        if pairs:
            mine, out_half = lax.optimization_barrier((mine, out_half))
            neighbours = [(i, i ^ 1) for i in range(fs_size)]
            out_next = lax.ppermute(out_half, "fs", neighbours)
            out_low = jnp.where(part == 0, out_half, out_next)
            out_high = jnp.where(part == 0, out_next, out_half)
        else:
            out_low, out_high = jnp.split(out_half, 2, axis=0)
        residual, normed_mid = out_projection(
            mine, received, mix_all, 2, out_low, 0, out_high, tokens, post_mix_gain, pre_ffn_gain
        )
        other_mid = lax.ppermute(normed_mid, "tp", swap)
        pieces = 2 if rows % 512 == 0 else 1
        size = rows // pieces
        returned = []
        for piece in range(pieces):
            part = ffn(lax.slice_in_dim(other_mid, piece * size, (piece + 1) * size), ffn_all)
            returned.append(lax.ppermute(part, "tp", swap))
        own_part = ffn(normed_mid, ffn_all)
        output = None
        for piece in range(pieces):
            output = finish(residual, own_part, returned[piece], post_ffn_gain, piece, output)
        return output
    else:
        everything = lax.all_gather(normed_in, "tp", axis=0, tiled=True)
        half = everything.shape[0] // 2
        first, second = mixer(
            place * 0, everything[:half], everything[half:], mix_all, conv_weight, w_rec, w_inp, slope
        )
        hidden = lax.all_to_all(
            jnp.concatenate([first, second], axis=0), "tp", split_axis=0, concat_axis=1, tiled=True
        )
        out_whole = lax.all_gather(mix_all[:, 2 * channels :], "tp", axis=1, tiled=True)
        mid_cols = hidden.shape[1] // 2
        residual, normed_mid = out_projection(
            hidden[:, :mid_cols], hidden[:, mid_cols:], out_whole, 0,
            out_whole[: out_whole.shape[0] // 2], 1, out_whole[out_whole.shape[0] // 2 :],
            tokens, post_mix_gain, pre_ffn_gain,
        )
        every_mid = lax.all_gather(normed_mid, "tp", axis=0, tiled=True)
        ffn_sum = lax.psum_scatter(
            ffn(every_mid, ffn_all), "tp", scatter_dimension=0, tiled=True
        ).astype(F32)
    return (residual.astype(F32) + normed(ffn_sum, post_ffn_gain)).astype(BF16)


def solution(mesh):
    return jax.shard_map(
        functools.partial(per_device, mesh.shape["tp"], mesh.shape["fs"]),
        mesh=mesh,
        in_specs=(
            P(("fs", "tp"), None),
            P(),
            P(),
            P(),
            P(),
            P("fs", "tp"),
            P("fs", "tp"),
            P(None, "tp"),
            P(None, "tp", None, None),
            P(None, "tp", None, None),
            P(None, "tp"),
            P("fs", "tp"),
            P("fs", "tp"),
            P("fs", "tp"),
            P("fs", "tp"),
        ),
        out_specs=P(("fs", "tp"), None),
        check_vma=False,
    )
```

```python
import functools

import jax
import jax.numpy as jnp
from jax import lax
from jax.experimental import pallas as pl
from jax.experimental.pallas import tpu as pltpu
from jax.sharding import PartitionSpec as P

EPS = 1e-06
SEGMENTS = 8
LANES = 128
F32 = jnp.float32
BF16 = jnp.bfloat16


def normed(values, gain):
    factor = lax.rsqrt(jnp.mean(values * values, axis=-1, keepdims=True) + EPS)
    return values * factor * gain


def tile_of(size, limit):
    tile = min(size, limit)
    while size % tile:
        tile -= LANES
    return tile


def cost(flops):
    return pl.CostEstimate(flops=flops, bytes_accessed=flops // 256, transcendentals=0)


def one_minus_exp(y):
    series = 1.0 + y * (1.0 / 6.0)
    for term in (5.0, 4.0, 3.0, 2.0):
        series = 1.0 + y * (1.0 / term) * series
    return jnp.where(y > -0.25, -y * series, 1.0 - jnp.exp(y))


def dot_nn(left, right):
    return jnp.dot(left, right, preferred_element_type=F32)


def dot_nt(left, right):
    return lax.dot_general(left, right, (((1,), (1,)), ((), ())), preferred_element_type=F32)


def mixer_kernel(
    place_ref, own_ref, other_ref, wb_ref, wg_ref, cw_ref, rec_ref, inp_ref, slope_ref,
    mine_ref, theirs_ref, branch_ref, gelu_ref, a0, b0, a1, b1, hf, hb,
):
    half = own_ref.shape[0]
    length = 2 * half
    steps = length // SEGMENTS
    blocks = rec_ref.shape[1]
    own_at = pl.multiple_of(place_ref[0] * half, half)
    other_at = pl.multiple_of((1 - place_ref[0]) * half, half)
    for source, start in ((own_ref, own_at), (other_ref, other_at)):
        rows = source[...]
        branch_ref[pl.ds(start, half), :] = dot_nn(rows, wb_ref[...]).astype(BF16).astype(F32)
        gelu_ref[pl.ds(start, half), :] = dot_nn(rows, wg_ref[...]).astype(BF16)
    row = lax.broadcasted_iota(jnp.int32, (length, LANES), 0)
    for block in range(blocks):
        cols = slice(block * LANES, (block + 1) * LANES)
        branch = branch_ref[:, cols]
        taps = cw_ref[:, cols].astype(F32)
        summed = taps[0:1] * jnp.where(row >= 2, pltpu.roll(branch, 2, 0), 0.0)
        summed = summed + taps[1:2] * jnp.where(row >= 1, pltpu.roll(branch, 1, 0), 0.0)
        summed = summed + taps[2:3] * branch
        summed = summed + taps[3:4] * jnp.where(
            row < length - 1, pltpu.roll(branch, length - 1, 0), 0.0
        )
        conv = summed.astype(BF16)
        conv_wide = conv.astype(F32)
        for direction, (a_ref, b_ref) in enumerate(((a0, b0), (a1, b1))):
            rate = jax.nn.sigmoid(dot_nn(conv, rec_ref[direction, block]))
            inflow = jax.nn.sigmoid(dot_nn(conv, inp_ref[direction, block]))
            log_a = rate * slope_ref[direction : direction + 1, cols]
            a_ref[block] = jnp.exp(log_a)
            b_ref[block] = jnp.sqrt(one_minus_exp(2.0 * log_a)) * inflow * conv_wide

    def at(step):
        return pl.ds(step, SEGMENTS, stride=steps)

    def advance(step, states, store):
        new = []
        back = steps - 1 - step
        for block in range(blocks):
            for ar, br, hr, where in ((a0, b0, hf, step), (a1, b1, hb, back)):
                state, product = states[len(new)]
                keep = ar[block, at(where), :]
                state = keep * state + br[block, at(where), :]
                if store:
                    hr[block, at(where), :] = state
                else:
                    product = product * keep
                new.append((state, product))
        return tuple(new)

    zero = jnp.zeros((SEGMENTS, LANES), F32)
    one = jnp.ones((SEGMENTS, LANES), F32)
    ends = lax.fori_loop(
        0, steps, lambda i, s: advance(i, s, False), ((zero, one),) * (2 * blocks), unroll=8
    )
    starts = []
    for index, (state, product) in enumerate(ends):
        order = list(range(SEGMENTS))
        if index % 2:
            order = order[::-1]
        rows = [None] * SEGMENTS
        carry = zero[0:1]
        for segment in order:
            rows[segment] = carry
            carry = state[segment : segment + 1] + product[segment : segment + 1] * carry
        starts.append((jnp.concatenate(rows, axis=0), zero))
    lax.fori_loop(0, steps, lambda i, s: advance(i, s, True), tuple(starts), unroll=8)
    for target, start in ((mine_ref, own_at), (theirs_ref, other_at)):
        for block in range(blocks):
            cols = slice(block * LANES, (block + 1) * LANES)
            states = hf[block, pl.ds(start, half), :] + hb[block, pl.ds(start, half), :]
            factor = jax.nn.gelu(gelu_ref[pl.ds(start, half), cols].astype(F32))
            target[:, cols] = (factor * states).astype(BF16)


def mixer(place, own, other, gathered, conv_weight, w_rec, w_inp, slope):
    half, width = own.shape
    channels = conv_weight.shape[1]
    group = tile_of(channels, 2 * LANES)
    blocks = group // LANES
    count = channels // group
    length = 2 * half
    wide = pltpu.VMEM((blocks, length, LANES), F32)
    whole = pl.BlockSpec((half, width), lambda j: (0, 0))
    maps = pl.BlockSpec((2, blocks, LANES, LANES), lambda j: (0, j, 0, 0))
    piece = pl.BlockSpec((half, group), lambda j: (0, j))
    return pl.pallas_call(
        mixer_kernel,
        grid=(count,),
        in_specs=[
            pl.BlockSpec(memory_space=pltpu.SMEM),
            whole,
            whole,
            pl.BlockSpec((width, group), lambda j: (0, j)),
            pl.BlockSpec((width, group), lambda j: (0, count + j)),
            pl.BlockSpec((conv_weight.shape[0], group), lambda j: (0, j)),
            maps,
            maps,
            pl.BlockSpec((2, group), lambda j: (0, j)),
        ],
        out_specs=[piece, piece],
        out_shape=[jax.ShapeDtypeStruct((half, channels), BF16)] * 2,
        scratch_shapes=[
            pltpu.VMEM((length, group), F32),
            pltpu.VMEM((length, group), BF16),
            wide, wide, wide, wide, wide, wide,
        ],
        compiler_params=pltpu.CompilerParams(vmem_limit_bytes=56 * 2**20),
        cost_estimate=cost(32 * length * width * channels),
        name="mixer",
    )(place, own, other, gathered, gathered, conv_weight, w_rec, w_inp, slope)


def out_kernel(
    ha_ref, hb_ref, wa_ref, wlow_ref, whigh_ref, tok_ref, gain_ref, mid_gain_ref, res_ref, mid_ref
):
    second = hb_ref[...]
    summed = dot_nt(ha_ref[...], wa_ref[...]) + jnp.concatenate(
        [dot_nt(second, wlow_ref[...]), dot_nt(second, whigh_ref[...])], axis=1
    )
    residual = (tok_ref[...].astype(F32) + normed(summed, gain_ref[...])).astype(BF16)
    res_ref[...] = residual
    mid_ref[...] = normed(residual.astype(F32), mid_gain_ref[...]).astype(BF16)


def out_projection(ha, hb, wa, wa_block, wlow, wb_block, whigh, tokens, gain, mid_gain):
    rows, width = tokens.shape
    tile = min(rows, 256)
    channels = ha.shape[1]
    hidden = pl.BlockSpec((tile, channels), lambda i: (i, 0))
    wide = pl.BlockSpec((tile, width), lambda i: (i, 0))
    gains = pl.BlockSpec((1, width), lambda i: (0, 0))
    return pl.pallas_call(
        out_kernel,
        grid=(rows // tile,),
        in_specs=[
            hidden,
            hidden,
            pl.BlockSpec((width, channels), lambda i: (0, wa_block)),
            pl.BlockSpec((width // 2, channels), lambda i: (0, wb_block)),
            pl.BlockSpec((width // 2, channels), lambda i: (0, wb_block)),
            wide,
            gains,
            gains,
        ],
        out_specs=[wide, wide],
        out_shape=[jax.ShapeDtypeStruct((rows, width), BF16)] * 2,
        compiler_params=pltpu.CompilerParams(vmem_limit_bytes=56 * 2**20),
        cost_estimate=cost(16 * rows * width * channels),
        name="out_projection",
    )(ha, hb, wa, wlow, whigh, tokens, gain[None], mid_gain[None])


def ffn_kernel(x_ref, gate_ref, up_ref, down_ref, out_ref, acc_ref):
    rows = x_ref[...]
    gate = dot_nn(rows, gate_ref[...])
    hidden = (gate * jax.nn.sigmoid(gate) * dot_nn(rows, up_ref[...])).astype(BF16)
    partial = dot_nt(hidden, down_ref[...])
    step = pl.program_id(0)
    last = pl.num_programs(0) - 1

    @pl.when(step == 0)
    def _():
        acc_ref[...] = partial

    @pl.when(step > 0)
    def _():
        acc_ref[...] += partial

    @pl.when(step == last)
    def _():
        out_ref[...] = acc_ref[...].astype(BF16)


def ffn(rows, gathered):
    count, width = rows.shape
    hidden_units = gathered.shape[1] // 3
    tile = tile_of(hidden_units, 512)
    tiles = hidden_units // tile
    whole = pl.BlockSpec((count, width), lambda j: (0, 0))
    return pl.pallas_call(
        ffn_kernel,
        grid=(tiles,),
        in_specs=[
            whole,
            pl.BlockSpec((width, tile), lambda j: (0, j)),
            pl.BlockSpec((width, tile), lambda j: (0, tiles + j)),
            pl.BlockSpec((width, tile), lambda j: (0, 2 * tiles + j)),
        ],
        out_specs=whole,
        out_shape=jax.ShapeDtypeStruct((count, width), BF16),
        scratch_shapes=[pltpu.VMEM((count, width), F32)],
        compiler_params=pltpu.CompilerParams(vmem_limit_bytes=56 * 2**20),
        cost_estimate=cost(6 * count * width * hidden_units),
        name="ffn",
    )(rows, gathered, gathered, gathered)


def finish_kernel(res_ref, own_ref, back_ref, gain_ref, *refs):
    summed = own_ref[...].astype(F32) + back_ref[...].astype(F32)
    layer = res_ref[...].astype(F32) + normed(summed, gain_ref[...])
    refs[-1][...] = layer.astype(BF16)


def finish(residual, own, back, gain, piece, earlier):
    size, width = back.shape
    tile = min(size, LANES)
    tiles = size // tile
    placed = pl.BlockSpec((tile, width), lambda i: (piece * tiles + i, 0))
    operands = [residual, own, back, gain[None]]
    specs = [
        placed,
        placed,
        pl.BlockSpec((tile, width), lambda i: (i, 0)),
        pl.BlockSpec((1, width), lambda i: (0, 0)),
    ]
    aliases = {}
    if earlier is not None:
        aliases = {len(operands): 0}
        operands.append(earlier)
        specs.append(pl.BlockSpec(memory_space=pl.ANY))
    return pl.pallas_call(
        finish_kernel,
        grid=(tiles,),
        in_specs=specs,
        out_specs=placed,
        out_shape=jax.ShapeDtypeStruct(residual.shape, BF16),
        input_output_aliases=aliases,
        name="finish",
    )(*operands)


def per_device(
    ranks,
    fs_size,
    tokens,
    pre_mix_gain,
    post_mix_gain,
    pre_ffn_gain,
    post_ffn_gain,
    w_branch,
    w_gelu,
    conv_weight,
    w_rec,
    w_inp,
    decay,
    out_weight_t,
    w_gate,
    w_up,
    down_weight_t,
):
    swap = [(0, 1), (1, 0)]
    rows = tokens.shape[0]
    mix_shard = jnp.concatenate([w_branch, w_gelu, out_weight_t], axis=1)
    ffn_shard = jnp.concatenate([w_gate, w_up, down_weight_t], axis=1)
    mix_all = lax.all_gather(mix_shard, "fs", axis=0, tiled=True)
    channels = w_branch.shape[1]
    stream = tokens.astype(F32)
    normed_in = normed(stream, pre_mix_gain).astype(BF16)
    if ranks == 2:
        other_in = lax.ppermute(normed_in, "tp", swap)
        mix_all, ffn_shard, other_in = lax.optimization_barrier((mix_all, ffn_shard, other_in))
    else:
        mix_all, ffn_shard = lax.optimization_barrier((mix_all, ffn_shard))
    ffn_all = lax.all_gather(ffn_shard, "fs", axis=0, tiled=True)
    slope = -8.0 * jax.nn.softplus(-decay)
    place = lax.axis_index("tp").astype(jnp.int32).reshape(1)
    if ranks == 2:
        lanes_at = 2 * channels
        width = mix_all.shape[0]
        pairs = fs_size % 2 == 0
        if pairs:
            part = lax.axis_index("fs").astype(jnp.int32) % 2
            out_half = lax.dynamic_slice(
                mix_all, (part * (width // 2), lanes_at), (width // 2, channels)
            )
        else:
            out_half = mix_all[:, lanes_at:]
        out_half = lax.ppermute(out_half, "tp", swap)
        mine, theirs = mixer(
            place, normed_in, other_in, mix_all, conv_weight, w_rec, w_inp, slope
        )
        received = lax.ppermute(theirs, "tp", swap)
        if pairs:
            mine, out_half = lax.optimization_barrier((mine, out_half))
            neighbours = [(i, i ^ 1) for i in range(fs_size)]
            out_next = lax.ppermute(out_half, "fs", neighbours)
            out_low = jnp.where(part == 0, out_half, out_next)
            out_high = jnp.where(part == 0, out_next, out_half)
        else:
            out_low, out_high = jnp.split(out_half, 2, axis=0)
        residual, normed_mid = out_projection(
            mine, received, mix_all, 2, out_low, 0, out_high, tokens, post_mix_gain, pre_ffn_gain
        )
        pieces = 2 if rows % 512 == 0 else 1
        size = rows // pieces
        returned = []
        crossed = [
            lax.ppermute(lax.slice_in_dim(normed_mid, i * size, (i + 1) * size), "tp", swap)
            for i in range(pieces)
        ]
        for piece in range(pieces):
            part = ffn(crossed[piece], ffn_all)
            returned.append(lax.ppermute(part, "tp", swap))
        own_part = ffn(normed_mid, ffn_all)
        output = None
        for piece in range(pieces):
            output = finish(residual, own_part, returned[piece], post_ffn_gain, piece, output)
        return output
    else:
        everything = lax.all_gather(normed_in, "tp", axis=0, tiled=True)
        half = everything.shape[0] // 2
        first, second = mixer(
            place * 0, everything[:half], everything[half:], mix_all, conv_weight, w_rec, w_inp, slope
        )
        hidden = lax.all_to_all(
            jnp.concatenate([first, second], axis=0), "tp", split_axis=0, concat_axis=1, tiled=True
        )
        out_whole = lax.all_gather(mix_all[:, 2 * channels :], "tp", axis=1, tiled=True)
        mid_cols = hidden.shape[1] // 2
        residual, normed_mid = out_projection(
            hidden[:, :mid_cols], hidden[:, mid_cols:], out_whole, 0,
            out_whole[: out_whole.shape[0] // 2], 1, out_whole[out_whole.shape[0] // 2 :],
            tokens, post_mix_gain, pre_ffn_gain,
        )
        every_mid = lax.all_gather(normed_mid, "tp", axis=0, tiled=True)
        ffn_sum = lax.psum_scatter(
            ffn(every_mid, ffn_all), "tp", scatter_dimension=0, tiled=True
        ).astype(F32)
    return (residual.astype(F32) + normed(ffn_sum, post_ffn_gain)).astype(BF16)


def solution(mesh):
    return jax.shard_map(
        functools.partial(per_device, mesh.shape["tp"], mesh.shape["fs"]),
        mesh=mesh,
        in_specs=(
            P(("fs", "tp"), None),
            P(),
            P(),
            P(),
            P(),
            P("fs", "tp"),
            P("fs", "tp"),
            P(None, "tp"),
            P(None, "tp", None, None),
            P(None, "tp", None, None),
            P(None, "tp"),
            P("fs", "tp"),
            P("fs", "tp"),
            P("fs", "tp"),
            P("fs", "tp"),
        ),
        out_specs=P(("fs", "tp"), None),
        check_vma=False,
    )
```
